1024 devices in a mesh: ep: 64 (over z, y), tp: 16 (over x, core).
Axes of the slice: x: 8, y: 8, z: 8, core: 2. Of those that a mesh axis runs over, the one named last changes fastest.
Arguments:
- tokens: bfloat16 [1024, 4096], P('ep'), may hold values from -6 to 6
- norm_gain: float32 [4096], replicated, may hold values from 0.1 to 1.9
- token_expert_index: int32 [1024, 4], P('ep'), may hold values from 0 to 63, as said below
- group_prob: float32 [1024], P('ep'), may hold values from 0.25 to 1
- expert_weight: float32 [1024, 4], P('ep'), may hold values from 0.05 to 1
- w_gate: bfloat16 [64, 4096, 2048], P('ep', None, 'tp'), may hold values from -0.09375 to 0.09375
- w_up: bfloat16 [64, 4096, 2048], P('ep', None, 'tp'), may hold values from -0.09375 to 0.09375
- w_down: bfloat16 [64, 2048, 4096], P('ep', 'tp'), may hold values from -0.125 to 0.125
Outputs:
- mixed: bfloat16 [1024, 4096], P('ep', 'tp')
The draws below stay inside these ranges and needn't reach their ends.
Inputs may be any that keep to these rules, and one draw needn't show every extreme that they name: `token_expert_index`: each row names 4 different experts, all of one group: the group g holds experts g * 32 to (g + 1) * 32 - 1. The 16 rows of one index of ep name any one expert at most 3 times.
All inputs are finite; a program needn't handle non-finite values.
Results may differ from the reference program's by a relative error of at most 0.019.
Values may be sent and summed in bfloat16 or wider, within the bound.
No kernel may reach another device: no remote copies, remote signals or barrier semaphores. Data moves between devices by JAX's collectives and lax.ppermute only.
A program may use at most 32 MiB of HBM per device.

```python
import math
import jax
import jax.numpy as jnp
from jax import lax

D = 4096
FF = 2048
TOK_DEV = 16
TOPK = 4
GROUPS = 2
EXPERTS = 64
CAP = 3
TOKENS = 1024
N_EP = 64
N_TP = 16


def draw_token_expert_index(key, part):
    blocks = TOKENS // TOK_DEV
    per_group = EXPERTS // GROUPS
    keys = jax.random.split(jax.random.fold_in(key, 11), 4)
    hottest = jax.random.randint(keys[0], (), 0, EXPERTS)
    favored_experts = jax.random.randint(keys[1], (EXPERTS,), 0, 4)
    extra_reward = jnp.where(favored_experts == 0, 3000, 0).astype(jnp.int32)
    group_draw = jax.random.randint(keys[2], (TOK_DEV, blocks), 0, GROUPS)
    noise = jax.random.randint(keys[3], (TOK_DEV, blocks, per_group), 0, 2000)
    block_ids = jnp.arange(blocks, dtype=jnp.int32)
    position = jnp.arange(TOK_DEV, dtype=jnp.int32)[:, None]
    after = jnp.broadcast_to((block_ids + 1) % EXPERTS, (TOK_DEV, blocks))
    across = jnp.broadcast_to((block_ids + EXPERTS // 2) % EXPERTS, (TOK_DEV, blocks))
    target = jnp.where(position == 0, after, jnp.where(position == 1, across, jnp.where((position >= 2) & (position < 2 + CAP), hottest, -1)))
    groups = jnp.where(target >= 0, target // per_group, group_draw)
    local = jnp.arange(per_group, dtype=jnp.int32)
    everyone = jnp.arange(EXPERTS, dtype=jnp.int32)

    def one_token(counts, inputs):
        grp, destination_index, coarse_estimate = inputs
        candidate_experts = grp[:, None] * per_group + local[None, :]
        used = jnp.take_along_axis(counts, candidate_experts, axis=1)
        baseline_score = coarse_estimate + extra_reward[candidate_experts] + jnp.where(candidate_experts == destination_index[:, None], 100000, 0)
        baseline_score = jnp.where(used >= CAP, -1, baseline_score)
        score = baseline_score * per_group + local[None, :]
        _, picked = lax.top_k(score, TOPK)
        chosen = (grp[:, None] * per_group + picked).astype(jnp.int32)
        counts = counts + jnp.sum((chosen[:, :, None] == everyone[None, None, :]).astype(jnp.int32), axis=1)
        return (counts, chosen)
    start = jnp.zeros((blocks, EXPERTS), jnp.int32)
    _, result = lax.scan(one_token, start, (groups, target, noise))
    return jnp.transpose(result, (1, 0, 2)).reshape(TOKENS, TOPK).astype(jnp.int32)


def levels(rng, shape, cuts, smallest, largest):
    def one(dim, blocks):
        draws = jax.random.uniform(jax.random.fold_in(jax.random.fold_in(rng, 6), dim), (blocks,), jnp.float32, smallest / len(cuts), largest / len(cuts))
        return jnp.repeat(jnp.exp(draws), shape[dim] // blocks).reshape((-1,) + (1,) * (len(shape) - dim - 1))

    level = one(*cuts[0])
    for cut in cuts[1:]:
        level = level * one(*cut)
    return level


def centred(stream_key, shape, scale, bound, cuts=(), kind=jnp.bfloat16):
    level = levels(stream_key, shape, cuts, -0.22, 0.18) if cuts else 1.0
    drawn = jax.random.normal(stream_key, shape, jnp.float32) * scale * level
    return jnp.minimum(jnp.maximum(drawn, -bound), bound).astype(kind)


def setup_inputs(seed: int = 0) -> dict:
    key_list = jax.random.split(jax.random.key(seed), 9)
    tokens = centred(key_list[0], (TOKENS, D), 1.0, 6.0, ((0, 64),))
    norm_gain = jnp.clip(1.0 + 0.18 * jax.random.normal(key_list[1], (D,), jnp.float32), 0.1, 1.9)
    token_expert_index = draw_token_expert_index(jax.random.fold_in(key_list[8], 71), 0)
    group_prob = jnp.clip(0.25 + 0.75 * jax.random.uniform(key_list[3], (TOKENS,), jnp.float32) ** levels(key_list[3], (TOKENS,), ((0, 64),), -0.2, 0.2), 0.25, 1.0)
    expert_weight = jnp.clip(jnp.exp(math.log(1.0) - 2.9957323 * jax.random.uniform(key_list[4], (TOKENS, TOPK), jnp.float32) ** levels(key_list[4], (TOKENS, TOPK), ((0, 64),), -0.2, 0.2)), 0.05, 1.0)
    w_gate = centred(key_list[5], (EXPERTS, D, FF), D ** -0.5, 0.09375, ((0, 64), (2, 16)))
    w_up = centred(key_list[6], (EXPERTS, D, FF), D ** -0.5, 0.09375, ((0, 64), (2, 16)))
    w_down = centred(key_list[7], (EXPERTS, FF, D), FF ** -0.5, 0.125, ((0, 64), (1, 16)))
    return {"tokens": tokens, "norm_gain": norm_gain, "token_expert_index": token_expert_index, "group_prob": group_prob, "expert_weight": expert_weight, "w_gate": w_gate, "w_up": w_up, "w_down": w_down}


def reference(tokens, norm_gain, token_expert_index, group_prob, expert_weight, w_gate, w_up, w_down):
    xf = tokens.astype(jnp.float32)
    normed = (xf * lax.rsqrt(lax.optimization_barrier(jnp.mean(xf * xf, axis=-1, keepdims=True)) + 1e-06) * norm_gain).astype(jnp.bfloat16)
    gates = group_prob[:, None] * expert_weight / lax.optimization_barrier(jnp.sum(expert_weight, axis=-1, keepdims=True))
    limit = N_EP * CAP
    padded = jnp.concatenate([normed, jnp.zeros((1, D), jnp.bfloat16)], axis=0)

    def one_expert(carry, inputs):
        gate_mat, up_mat, down_mat, number = inputs
        hits = token_expert_index == number
        weight = lax.optimization_barrier(jnp.sum(jnp.where(hits, gates, jnp.float32(0.0)), axis=1))
        weight = jnp.concatenate([weight, jnp.zeros((1,), jnp.float32)])
        rows = jnp.nonzero(jnp.any(hits, axis=1), size=limit, fill_value=TOKENS)[0].astype(jnp.int32)
        chosen = padded[rows]
        gate = jnp.dot(chosen, gate_mat, preferred_element_type=jnp.float32)
        upper = jnp.dot(chosen, up_mat, preferred_element_type=jnp.float32)
        hidden = (jax.nn.silu(gate) * upper).astype(jnp.bfloat16)
        blocks = hidden.reshape(limit, N_TP, FF // N_TP).astype(jnp.float32)
        downs = down_mat.reshape(N_TP, FF // N_TP, D).astype(jnp.float32)
        parts = jnp.einsum('rnf,nfd->nrd', blocks, downs).astype(jnp.bfloat16)
        parts = lax.optimization_barrier(parts).astype(jnp.float32)
        output = lax.optimization_barrier(jnp.sum(parts, axis=0)).astype(jnp.bfloat16).astype(jnp.float32)
        carry = carry.at[rows].add(output * weight[rows][:, None])
        return (carry, None)
    start = jnp.zeros((TOKENS + 1, D), jnp.float32)
    numbers = jnp.arange(EXPERTS, dtype=jnp.int32)
    total, _ = lax.scan(one_expert, start, (w_gate, w_up, w_down, numbers))
    return total[:TOKENS].astype(jnp.bfloat16)
```

```python
import jax
import jax.numpy as jnp
from jax import lax
from jax.sharding import PartitionSpec as P

GROUPS = 2


def joined_along(blocks, dim):
    shape = list(blocks.shape[1:])
    shape[dim] *= blocks.shape[0]
    return jnp.moveaxis(blocks, 0, dim).reshape(shape)


def in_blocks(x, dim, size):
    before, after = (x.shape[:dim], x.shape[dim + 1 :])
    return jnp.moveaxis(x.reshape(*before, size, -1, *after), dim, 0)


def body(tokens, norm_gain, token_expert_index, group_prob, expert_weight, w_gate, w_up, w_down):
    rows_here, width = tokens.shape
    topk = token_expert_index.shape[1]
    experts = lax.axis_size("ep")
    tp_count = lax.axis_size("tp")
    per_group = experts // GROUPS
    capacity = min(rows_here, max(2, rows_here * topk // max(per_group - topk, 1) + 1))
    xf = tokens.astype(jnp.float32)
    normed = (xf * lax.rsqrt(jnp.mean(xf * xf, axis=-1, keepdims=True) + 1e-06) * norm_gain).astype(
        jnp.bfloat16
    )
    gates = group_prob[:, None] * expert_weight / jnp.sum(expert_weight, axis=-1, keepdims=True)
    flattened_index = token_expert_index.reshape(-1)
    onehot = (flattened_index[:, None] == jnp.arange(experts, dtype=jnp.int32)[None, :]).astype(
        jnp.int32
    )
    earlier = jnp.cumsum(onehot, axis=0) - onehot
    slot_rank = jnp.sum(earlier * onehot, axis=1)
    place = flattened_index * capacity + slot_rank
    slots_total = experts * capacity
    select = (jnp.arange(slots_total, dtype=jnp.int32)[:, None] == place[None, :]).astype(
        jnp.float32
    )
    select = jnp.sum(select.reshape(slots_total, rows_here, topk), axis=2).astype(jnp.bfloat16)
    outgoing = jnp.dot(select, normed, preferred_element_type=jnp.float32).astype(jnp.bfloat16)
    tp_index = lax.axis_index("tp")
    share = width // tp_count
    piece = lax.dynamic_slice_in_dim(outgoing, tp_index * share, share, 1)
    arrived = lax.all_to_all(piece, "ep", split_axis=0, concat_axis=0, tiled=True)
    arrived = joined_along(lax.all_gather(arrived, "tp", axis=0), 1)
    gate = jnp.dot(arrived, w_gate[0], preferred_element_type=jnp.float32)
    upper = jnp.dot(arrived, w_up[0], preferred_element_type=jnp.float32)
    hidden = (jax.nn.silu(gate) * upper).astype(jnp.bfloat16)
    partial_out = jnp.dot(hidden, w_down[0], preferred_element_type=jnp.float32)
    blocks = in_blocks(partial_out.astype(jnp.bfloat16), 1, tp_count)
    mine = lax.psum_scatter(blocks, "tp", scatter_dimension=0, tiled=False)
    returned = lax.all_to_all(mine, "ep", split_axis=0, concat_axis=0, tiled=True)
    picked = returned[place].astype(jnp.float32).reshape(rows_here, topk, share)
    mixed = jnp.sum(picked * gates[:, :, None], axis=1)
    return mixed.astype(jnp.bfloat16)


def solution(mesh):
    return jax.shard_map(
        body,
        mesh=mesh,
        in_specs=(
            P("ep", None),
            P(),
            P("ep", None),
            P("ep"),
            P("ep", None),
            P("ep", None, "tp"),
            P("ep", None, "tp"),
            P("ep", "tp", None),
        ),
        out_specs=P("ep", "tp"),
        check_vma=False,
    )
```

```python
import jax
import jax.numpy as jnp
from jax import lax
from jax.sharding import PartitionSpec as P

GROUPS = 2


def body(tokens, norm_gain, token_expert_index, group_prob, expert_weight, w_gate, w_up, w_down):
    rows_here, width = tokens.shape
    topk = token_expert_index.shape[1]
    experts = lax.axis_size("ep")
    tp_count = lax.axis_size("tp")
    chips = tp_count // 2
    share = width // tp_count
    half = width // 2
    core = lax.axis_index("tp") % 2
    swap = [(i, i ^ 1) for i in range(tp_count)]
    same_core = [[2 * i + c for i in range(chips)] for c in range(2)]
    per_group = experts // GROUPS
    capacity = min(rows_here, max(2, rows_here * topk // max(per_group - topk, 1) + 1))
    slots_total = experts * capacity
    xf = tokens.astype(jnp.float32)
    normed = (xf * lax.rsqrt(jnp.mean(xf * xf, axis=-1, keepdims=True) + 1e-06) * norm_gain).astype(
        jnp.bfloat16
    )
    gates = group_prob[:, None] * expert_weight / jnp.sum(expert_weight, axis=-1, keepdims=True)
    flattened_index = token_expert_index.reshape(-1)
    onehot = (flattened_index[:, None] == jnp.arange(experts, dtype=jnp.int32)[None, :]).astype(
        jnp.int32
    )
    earlier = jnp.cumsum(onehot, axis=0) - onehot
    slot_rank = jnp.sum(earlier * onehot, axis=1)
    place = flattened_index * capacity + slot_rank
    at_place = jnp.arange(slots_total, dtype=jnp.int32)[:, None] == place[None, :]
    select = jnp.sum(
        at_place.astype(jnp.float32).reshape(slots_total, rows_here, topk), axis=2
    ).astype(jnp.bfloat16)

    mine_in = lax.dynamic_slice_in_dim(normed.reshape(rows_here, chips, 2, share), core, 1, 2)
    outgoing = jnp.dot(
        select, mine_in.reshape(rows_here, half), preferred_element_type=jnp.float32
    ).astype(jnp.bfloat16)
    outgoing = outgoing.reshape(experts, capacity * chips, share)
    arrived = lax.all_to_all(outgoing, "ep", split_axis=0, concat_axis=0, tiled=True)
    other = lax.ppermute(arrived, "tp", swap)
    arrived = arrived.reshape(slots_total, half)
    other = other.reshape(slots_total, half)

    def rows_of(w, which):
        w = w.reshape(chips, 2, share, w.shape[1])
        return lax.dynamic_slice_in_dim(w, which, 1, 1).reshape(half, w.shape[3])

    def into(w):
        a = jnp.dot(arrived, rows_of(w, core), preferred_element_type=jnp.float32)
        b = jnp.dot(other, rows_of(w, 1 - core), preferred_element_type=jnp.float32)
        return a + b

    hidden = (jax.nn.silu(into(w_gate[0])) * into(w_up[0])).astype(jnp.bfloat16)

    down = w_down[0].reshape(-1, chips, 2, share)

    def out_of(which):
        w = lax.dynamic_slice_in_dim(down, which, 1, 2).reshape(-1, half)
        return jnp.dot(hidden, w, preferred_element_type=jnp.float32).astype(jnp.bfloat16)

    theirs = lax.ppermute(out_of(1 - core), "tp", swap)
    mine = (out_of(core).astype(jnp.float32) + theirs.astype(jnp.float32)).astype(jnp.bfloat16)
    mine = mine.reshape(experts, capacity * chips, share)
    returned = lax.all_to_all(mine, "ep", split_axis=0, concat_axis=0, tiled=True)
    returned = returned.reshape(slots_total, half)
    weigh = jnp.sum(
        (at_place.astype(jnp.float32) * gates.reshape(-1)[None, :]).reshape(
            slots_total, rows_here, topk
        ),
        axis=2,
    )
    partial_mix = jnp.dot(
        weigh.T,
        returned.astype(jnp.float32),
        precision=lax.Precision.HIGHEST,
        preferred_element_type=jnp.float32,
    ).astype(jnp.bfloat16)
    blocks = jnp.moveaxis(partial_mix.reshape(rows_here, chips, share), 1, 0)
    parts = lax.all_to_all(
        blocks, "tp", split_axis=0, concat_axis=0, tiled=True, axis_index_groups=same_core
    )
    return parts.astype(jnp.float32).sum(axis=0).astype(jnp.bfloat16)


def solution(mesh):
    return jax.shard_map(
        body,
        mesh=mesh,
        in_specs=(
            P("ep", None),
            P(),
            P("ep", None),
            P("ep"),
            P("ep", None),
            P("ep", None, "tp"),
            P("ep", None, "tp"),
            P("ep", "tp", None),
        ),
        out_specs=P("ep", "tp"),
        check_vma=False,
    )
```

```python
import jax
import jax.numpy as jnp
from jax import lax
from jax.experimental import pallas as pl
from jax.experimental.pallas import tpu as pltpu
from jax.sharding import PartitionSpec as P

GROUPS = 2
BLOCK = 256
LANES = 128


def dispatch_kernel(core_ref, index_ref, tokens_ref, gain_ref, out_ref, count_ref, *lanes):
    tokens, width = tokens_ref.shape
    experts, _, chips, share = out_ref.shape
    topk = index_ref.shape[0] // tokens
    core = core_ref[0]
    xf = tokens_ref[...].astype(jnp.float32)
    scale = lax.rsqrt(jnp.mean(xf * xf, axis=-1, keepdims=True) + 1e-06)
    for b in range(chips):
        at = pl.multiple_of((2 * b + core) * share, share)
        block = tokens_ref[:, pl.ds(at, share)].astype(jnp.float32)
        block = block * scale * gain_ref[:, pl.ds(at, share)]
        for i, ref in enumerate(lanes):
            ref[pl.ds(b, tokens, stride=chips), :] = block[:, i * LANES : (i + 1) * LANES]
    out_ref[...] = jnp.zeros_like(out_ref)

    def clear(e, _):
        count_ref[e] = 0

    lax.fori_loop(0, experts, clear, None, unroll=8)

    def token(t, _):
        here = pl.ds(pl.multiple_of(t * chips, chips), chips)
        row = jnp.concatenate([ref[here, :] for ref in lanes], axis=1).astype(jnp.bfloat16)
        for k in range(topk):
            e = index_ref[t * topk + k]
            rank = count_ref[e]
            count_ref[e] = rank + 1
            out_ref[e, rank] = row

    lax.fori_loop(0, tokens, token, None)


def block_at(b, which):
    return pl.ds(pl.multiple_of((2 * b + which) * BLOCK, BLOCK), BLOCK)


def fetch(which, sources, buffer, sems):
    copies = []
    for b in range(buffer.shape[1]):
        pair = []
        for i, source in enumerate(sources):
            pair.append(
                pltpu.make_async_copy(source.at[block_at(b, which)], buffer.at[i, b], sems.at[i, b])
            )
            pair[-1].start()
        copies.append(pair)
    return copies


def project(x_ref, copies, buffer, gate, up):
    for b, pair in enumerate(copies):
        x = x_ref[:, b * BLOCK : (b + 1) * BLOCK]
        for copy in pair:
            copy.wait()
        gate += jnp.dot(x, buffer[0, b], preferred_element_type=jnp.float32)
        up += jnp.dot(x, buffer[1, b], preferred_element_type=jnp.float32)
    return gate, up


def own_kernel(core_ref, x_ref, gate_ref, up_ref, sums_ref, buffer, sems):
    copies = fetch(core_ref[0], (gate_ref, up_ref), buffer, sems)
    zero = jnp.zeros(sums_ref.shape[1:], jnp.float32)
    sums_ref[0], sums_ref[1] = project(x_ref, copies, buffer, zero, zero)


def other_kernel(
    core_ref, x_ref, sums_ref, gate_ref, up_ref, down_ref, keep_ref, send_ref, buffer, sems, down, sem
):
    core = core_ref[0]
    copies = fetch(1 - core, (gate_ref, up_ref), buffer, sems)
    rest = pltpu.make_async_copy(down_ref, down, sem)
    rest.start()
    gate, up = project(x_ref, copies, buffer, sums_ref[0], sums_ref[1])
    hidden = (gate * jax.nn.sigmoid(gate) * up).astype(jnp.bfloat16)
    rest.wait()
    for ref, which in ((send_ref, 1 - core), (keep_ref, core)):
        for b in range(buffer.shape[1]):
            out = jnp.dot(hidden, down[:, block_at(b, which)], preferred_element_type=jnp.float32)
            ref[:, b * BLOCK : (b + 1) * BLOCK] = out.astype(jnp.bfloat16)


GRANT = pltpu.CompilerParams(vmem_limit_bytes=16 * 2**20)
SMEM = pl.BlockSpec(memory_space=pltpu.SMEM)
VMEM = pl.BlockSpec(memory_space=pltpu.VMEM)
HBM = pl.BlockSpec(memory_space=pltpu.HBM)


def in_vmem(x):
    return pltpu.with_memory_space_constraint(x, pltpu.VMEM)


def in_hbm(x):
    return pltpu.with_memory_space_constraint(x, pltpu.HBM)


def body(tokens, norm_gain, token_expert_index, group_prob, expert_weight, w_gate, w_up, w_down):
    rows_here, width = tokens.shape
    topk = token_expert_index.shape[1]
    experts = lax.axis_size("ep")
    tp_count = lax.axis_size("tp")
    chips = tp_count // 2
    share = width // tp_count
    half = width // 2
    core = lax.axis_index("tp") % 2
    swap = [(i, i ^ 1) for i in range(tp_count)]
    same_core = [[2 * i + c for i in range(chips)] for c in range(2)]
    per_group = experts // GROUPS
    capacity = min(rows_here, max(2, rows_here * topk // max(per_group - topk, 1) + 1))
    slots_total = experts * capacity
    gates = group_prob[:, None] * expert_weight / jnp.sum(expert_weight, axis=-1, keepdims=True)
    flattened_index = token_expert_index.reshape(-1)
    onehot = (flattened_index[:, None] == jnp.arange(experts, dtype=jnp.int32)[None, :]).astype(
        jnp.int32
    )
    earlier = jnp.cumsum(onehot, axis=0) - onehot
    slot_rank = jnp.sum(earlier * onehot, axis=1)
    place = flattened_index * capacity + slot_rank
    at_place = jnp.arange(slots_total, dtype=jnp.int32)[:, None] == place[None, :]
    core_id = core.astype(jnp.int32).reshape(1)
    outgoing = pl.pallas_call(
        dispatch_kernel,
        out_shape=pltpu.VMEM((experts, capacity, chips, share), jnp.bfloat16),
        in_specs=[SMEM, SMEM, VMEM, VMEM],
        out_specs=VMEM,
        scratch_shapes=[
            pltpu.SMEM((experts,), jnp.int32),
            *[pltpu.VMEM((rows_here * chips, LANES), jnp.float32)] * (share // LANES),
        ],
        compiler_params=GRANT,
        name="dispatch",
    )(core_id, flattened_index, tokens, norm_gain[None, :])
    outgoing = outgoing.reshape(experts, capacity * chips, share)
    arrived = lax.all_to_all(outgoing, "ep", split_axis=0, concat_axis=0, tiled=True)
    other = lax.ppermute(arrived, "tp", swap)
    arrived = arrived.reshape(slots_total, half)
    other = other.reshape(slots_total, half)

    units = w_gate.shape[2]
    both = pltpu.VMEM((slots_total, half), jnp.bfloat16)
    weights = [
        pltpu.VMEM((2, chips, share, units), jnp.bfloat16),
        pltpu.SemaphoreType.DMA((2, chips)),
    ]
    sums = pl.pallas_call(
        own_kernel,
        out_shape=pltpu.VMEM((2, slots_total, units), jnp.float32),
        in_specs=[SMEM, VMEM, HBM, HBM],
        out_specs=VMEM,
        scratch_shapes=weights,
        compiler_params=GRANT,
        name="own_half",
    )(core_id, in_vmem(arrived), in_hbm(w_gate[0]), in_hbm(w_up[0]))
    keep, send = pl.pallas_call(
        other_kernel,
        out_shape=(both, both),
        in_specs=[SMEM, VMEM, VMEM, HBM, HBM, HBM],
        out_specs=(VMEM, VMEM),
        scratch_shapes=weights
        + [pltpu.VMEM((units, width), jnp.bfloat16), pltpu.SemaphoreType.DMA],
        compiler_params=GRANT,
        name="other_half",
    )(core_id, in_vmem(other), in_vmem(sums), *(in_hbm(w[0]) for w in (w_gate, w_up, w_down)))
    theirs = lax.ppermute(send, "tp", swap)
    mine = (keep.astype(jnp.float32) + theirs.astype(jnp.float32)).astype(jnp.bfloat16)
    mine = mine.reshape(experts, capacity * chips, share)
    returned = lax.all_to_all(mine, "ep", split_axis=0, concat_axis=0, tiled=True)
    returned = returned.reshape(slots_total, half)
    weigh = jnp.sum(
        (at_place.astype(jnp.float32) * gates.reshape(-1)[None, :]).reshape(
            slots_total, rows_here, topk
        ),
        axis=2,
    )
    partial_mix = jnp.dot(
        weigh.T,
        returned.astype(jnp.float32),
        precision=lax.Precision.HIGHEST,
        preferred_element_type=jnp.float32,
    ).astype(jnp.bfloat16)
    blocks = jnp.moveaxis(partial_mix.reshape(rows_here, chips, share), 1, 0)
    parts = lax.all_to_all(
        blocks, "tp", split_axis=0, concat_axis=0, tiled=True, axis_index_groups=same_core
    )
    return parts.astype(jnp.float32).sum(axis=0).astype(jnp.bfloat16)


def solution(mesh):
    return jax.shard_map(
        body,
        mesh=mesh,
        in_specs=(
            P("ep", None),
            P(),
            P("ep", None),
            P("ep"),
            P("ep", None),
            P("ep", None, "tp"),
            P("ep", None, "tp"),
            P("ep", "tp", None),
        ),
        out_specs=P("ep", "tp"),
        check_vma=False,
    )
```

```python
import jax
import jax.numpy as jnp
from jax import lax
from jax.experimental import pallas as pl
from jax.experimental.pallas import tpu as pltpu
from jax.sharding import PartitionSpec as P

GROUPS = 2
BLOCK = 256
LANES = 128


def block_at(b, which):
    return pl.ds(pl.multiple_of((2 * b + which) * BLOCK, BLOCK), BLOCK)


def into_blocks(gate_hbm, up_hbm, which, out_ref, sems):
    return [
        pltpu.make_async_copy(hbm.at[block_at(b, which)], out_ref.at[i, b], sems.at[i, b])
        for b in range(out_ref.shape[1])
        for i, hbm in enumerate((gate_hbm, up_hbm))
    ]


def columns(hbm, which, out_ref, sems):
    return [
        pltpu.make_async_copy(
            hbm.at[:, block_at(b, which)], out_ref.at[:, b * BLOCK : (b + 1) * BLOCK], sems.at[b]
        )
        for b in range(out_ref.shape[1] // BLOCK)
    ]


def dispatch_kernel(
    core_ref, index_ref, tokens_hbm, gain_hbm, gate_hbm, up_hbm, down_hbm,
    out_ref, near_ref, send_ref,
    tokens_ref, gain_ref, count_ref, sems, near_sems, down_sems, *lanes,
):
    core = core_ref[0]
    tokens, width = tokens_ref.shape
    experts, _, chips, share = out_ref.shape
    topk = index_ref.shape[0]
    first = [
        pltpu.make_async_copy(tokens_hbm, tokens_ref, sems.at[0]),
        pltpu.make_async_copy(gain_hbm, gain_ref, sems.at[1]),
    ]
    rest = into_blocks(gate_hbm, up_hbm, core, near_ref, near_sems)
    rest += columns(down_hbm, 1 - core, send_ref, down_sems)
    for copy in first + rest:
        copy.start()
    out_ref[...] = jnp.zeros_like(out_ref)

    def clear(e, _):
        count_ref[e] = 0

    lax.fori_loop(0, experts, clear, None, unroll=8)
    for copy in first:
        copy.wait()
    xf = tokens_ref[...].astype(jnp.float32)
    scale = lax.rsqrt(jnp.mean(xf * xf, axis=-1, keepdims=True) + 1e-06)
    for b in range(chips):
        at = block_at(b, core)
        block = tokens_ref[:, at].astype(jnp.float32) * scale * gain_ref[:, at]
        for i, ref in enumerate(lanes):
            ref[pl.ds(b, tokens, stride=chips), :] = block[:, i * LANES : (i + 1) * LANES]

    def token(t, _):
        here = pl.ds(pl.multiple_of(t * chips, chips), chips)
        row = jnp.concatenate([ref[here, :] for ref in lanes], axis=1).astype(jnp.bfloat16)
        for k in range(topk):
            e = index_ref[k, t]
            rank = count_ref[e]
            count_ref[e] = rank + 1
            out_ref[e, rank] = row

    lax.fori_loop(0, tokens, token, None)
    for copy in rest:
        copy.wait()


def project(x_ref, weights_ref, gate, up):
    for b in range(weights_ref.shape[1]):
        x = x_ref[:, b * BLOCK : (b + 1) * BLOCK]
        gate += jnp.dot(x, weights_ref[0, b], preferred_element_type=jnp.float32)
        up += jnp.dot(x, weights_ref[1, b], preferred_element_type=jnp.float32)
    return gate, up


def own_kernel(
    core_ref, x_ref, near_ref, gate_hbm, up_hbm, down_hbm, sums_ref, far_ref, keep_ref, sems, down_sems
):
    core = core_ref[0]
    copies = into_blocks(gate_hbm, up_hbm, 1 - core, far_ref, sems)
    copies += columns(down_hbm, core, keep_ref, down_sems)
    for copy in copies:
        copy.start()
    zero = jnp.zeros(sums_ref.shape[1:], jnp.float32)
    sums_ref[0], sums_ref[1] = project(x_ref, near_ref, zero, zero)
    for copy in copies:
        copy.wait()


def other_kernel(x_ref, sums_ref, far_ref, hidden_ref):
    gate, up = project(x_ref, far_ref, sums_ref[0], sums_ref[1])
    hidden_ref[...] = (gate * jax.nn.sigmoid(gate) * up).astype(jnp.bfloat16)


def output_kernel(own_ref, theirs_ref, keep_ref, crossed_ref, out_ref, *lanes):
    slots, chips, share = out_ref.shape
    own, theirs = own_ref[...], theirs_ref[...]
    for b in range(chips):
        at = pl.ds(b * BLOCK, BLOCK)
        out = jnp.dot(own, keep_ref[:, at], preferred_element_type=jnp.float32)
        out += jnp.dot(theirs, crossed_ref[:, at], preferred_element_type=jnp.float32)
        for i, ref in enumerate(lanes):
            ref[pl.ds(b, slots, stride=chips), :] = out[:, i * LANES : (i + 1) * LANES]
    for i, ref in enumerate(lanes):
        part = ref[...].reshape(slots, chips, LANES).astype(jnp.bfloat16)
        out_ref[:, :, i * LANES : (i + 1) * LANES] = part


GRANT = pltpu.CompilerParams(vmem_limit_bytes=16 * 2**20)
SMEM = pl.BlockSpec(memory_space=pltpu.SMEM)
VMEM = pl.BlockSpec(memory_space=pltpu.VMEM)
HBM = pl.BlockSpec(memory_space=pltpu.HBM)


def in_vmem(x):
    return pltpu.with_memory_space_constraint(x, pltpu.VMEM)


def in_hbm(x):
    return pltpu.with_memory_space_constraint(x, pltpu.HBM)


def body(tokens, norm_gain, token_expert_index, group_prob, expert_weight, w_gate, w_up, w_down):
    rows_here, width = tokens.shape
    topk = token_expert_index.shape[1]
    experts = lax.axis_size("ep")
    tp_count = lax.axis_size("tp")
    chips = tp_count // 2
    share = width // tp_count
    half = width // 2
    units = w_gate.shape[2]
    core = lax.axis_index("tp") % 2
    swap = [(i, i ^ 1) for i in range(tp_count)]
    same_core = [[2 * i + c for i in range(chips)] for c in range(2)]
    per_group = experts // GROUPS
    capacity = min(rows_here, max(2, rows_here * topk // max(per_group - topk, 1) + 1))
    slots_total = experts * capacity
    gates = group_prob[:, None] * expert_weight / jnp.sum(expert_weight, axis=-1, keepdims=True)
    flattened_index = token_expert_index.reshape(-1)
    onehot = (flattened_index[:, None] == jnp.arange(experts, dtype=jnp.int32)[None, :]).astype(
        jnp.int32
    )
    earlier = jnp.cumsum(onehot, axis=0) - onehot
    slot_rank = jnp.sum(earlier * onehot, axis=1)
    place = flattened_index * capacity + slot_rank
    at_place = jnp.arange(slots_total, dtype=jnp.int32)[:, None] == place[None, :]

    weigh = jnp.sum(
        (at_place.astype(jnp.float32) * gates.reshape(-1)[None, :]).reshape(
            slots_total, rows_here, topk
        ),
        axis=2,
    )

    core_id = core.astype(jnp.int32).reshape(1)
    blocks = pltpu.VMEM((2, chips, share, units), jnp.bfloat16)
    part = pltpu.VMEM((units, half), jnp.bfloat16)
    block_sems = pltpu.SemaphoreType.DMA((2, chips))
    part_sems = pltpu.SemaphoreType.DMA((chips,))
    weights = [in_hbm(w[0]) for w in (w_gate, w_up, w_down)]
    outgoing, near, down_send = pl.pallas_call(
        dispatch_kernel,
        out_shape=(pltpu.VMEM((experts, capacity, chips, share), jnp.bfloat16), blocks, part),
        in_specs=[SMEM, SMEM, HBM, HBM, HBM, HBM, HBM],
        out_specs=(VMEM,) * 3,
        scratch_shapes=[
            pltpu.VMEM((rows_here, width), jnp.bfloat16),
            pltpu.VMEM((1, width), jnp.float32),
            pltpu.SMEM((experts,), jnp.int32),
            pltpu.SemaphoreType.DMA((2,)),
            block_sems,
            part_sems,
            *[pltpu.VMEM((rows_here * chips, LANES), jnp.float32)] * (share // LANES),
        ],
        compiler_params=GRANT,
        name="dispatch",
    )(core_id, token_expert_index.T, in_hbm(tokens), in_hbm(norm_gain[None, :]), *weights)
    outgoing = outgoing.reshape(experts, capacity * chips, share)
    crossed = lax.ppermute(down_send, "tp", swap)
    arrived = lax.all_to_all(outgoing, "ep", split_axis=0, concat_axis=0, tiled=True)
    arrived, crossed, weigh = lax.optimization_barrier((arrived, crossed, weigh))
    arrived = arrived.reshape(slots_total, half)
    other = lax.ppermute(arrived, "tp", swap)
    sums, far, down_keep = pl.pallas_call(
        own_kernel,
        out_shape=(pltpu.VMEM((2, slots_total, units), jnp.float32), blocks, part),
        in_specs=[SMEM, VMEM, VMEM, HBM, HBM, HBM],
        out_specs=(VMEM,) * 3,
        scratch_shapes=[block_sems, part_sems],
        compiler_params=GRANT,
        name="own_half",
    )(core_id, in_vmem(arrived), in_vmem(near), *weights)
    hidden = pl.pallas_call(
        other_kernel,
        out_shape=pltpu.VMEM((slots_total, units), jnp.bfloat16),
        in_specs=[VMEM, VMEM, VMEM],
        out_specs=VMEM,
        compiler_params=GRANT,
        name="other_half",
    )(*(in_vmem(x) for x in (other, sums, far)))
    theirs = lax.ppermute(hidden, "tp", swap)
    mine = pl.pallas_call(
        output_kernel,
        out_shape=pltpu.VMEM((slots_total, chips, share), jnp.bfloat16),
        in_specs=[VMEM, VMEM, VMEM, VMEM],
        out_specs=VMEM,
        scratch_shapes=[pltpu.VMEM((slots_total * chips, LANES), jnp.float32)] * (share // LANES),
        compiler_params=GRANT,
        name="output",
    )(*(in_vmem(x) for x in (hidden, theirs, down_keep, crossed)))
    mine = mine.reshape(experts, capacity * chips, share)
    returned = lax.all_to_all(mine, "ep", split_axis=0, concat_axis=0, tiled=True)
    returned = returned.reshape(slots_total, half)
    partial_mix = jnp.dot(
        weigh.T,
        returned.astype(jnp.float32),
        precision=lax.Precision.HIGHEST,
        preferred_element_type=jnp.float32,
    ).astype(jnp.bfloat16)
    blocks = jnp.moveaxis(partial_mix.reshape(rows_here, chips, share), 1, 0)
    parts = lax.all_to_all(
        blocks, "tp", split_axis=0, concat_axis=0, tiled=True, axis_index_groups=same_core
    )
    return parts.astype(jnp.float32).sum(axis=0).astype(jnp.bfloat16)


def solution(mesh):
    return jax.shard_map(
        body,
        mesh=mesh,
        in_specs=(
            P("ep", None),
            P(),
            P("ep", None),
            P("ep"),
            P("ep", None),
            P("ep", None, "tp"),
            P("ep", None, "tp"),
            P("ep", "tp", None),
        ),
        out_specs=P("ep", "tp"),
        check_vma=False,
    )
```

```python
import jax
import jax.numpy as jnp
from jax import lax
from jax.experimental import pallas as pl
from jax.experimental.pallas import tpu as pltpu
from jax.sharding import PartitionSpec as P

GROUPS = 2
BLOCK = 256
LANES = 128


def block_at(b, which):
    return pl.ds(pl.multiple_of((2 * b + which) * BLOCK, BLOCK), BLOCK)


def into_blocks(gate_hbm, up_hbm, which, out_ref, sems):
    return [
        pltpu.make_async_copy(hbm.at[block_at(b, which)], out_ref.at[i, b], sems.at[i, b])
        for b in range(out_ref.shape[1])
        for i, hbm in enumerate((gate_hbm, up_hbm))
    ]


def columns(hbm, which, out_ref, sems):
    return [
        pltpu.make_async_copy(
            hbm.at[:, block_at(b, which)], out_ref.at[:, b * BLOCK : (b + 1) * BLOCK], sems.at[b]
        )
        for b in range(out_ref.shape[1] // BLOCK)
    ]


def dispatch_kernel(
    index_hbm, tokens_hbm, gain_hbm,
    out_ref,
    index_ref, tokens_ref, gain_ref, count_ref, sems, *lanes,
):
    core = lax.axis_index("tp") % 2
    tokens, width = tokens_ref.shape
    experts, _, chips, share = out_ref.shape
    topk = index_ref.shape[0]
    copies = [
        pltpu.make_async_copy(hbm, ref, sems.at[i])
        for i, (hbm, ref) in enumerate(
            ((tokens_hbm, tokens_ref), (index_hbm, index_ref), (gain_hbm, gain_ref))
        )
    ]
    for copy in copies:
        copy.start()
    out_ref[...] = jnp.zeros_like(out_ref)

    def clear(e, _):
        count_ref[e] = 0

    lax.fori_loop(0, experts, clear, None, unroll=8)
    for copy in copies:
        copy.wait()
    xf = tokens_ref[...].astype(jnp.float32)
    scale = lax.rsqrt(jnp.mean(xf * xf, axis=-1, keepdims=True) + 1e-06)
    for b in range(chips):
        at = block_at(b, core)
        block = tokens_ref[:, at].astype(jnp.float32) * scale * gain_ref[:, at]
        for i, ref in enumerate(lanes):
            ref[pl.ds(b, tokens, stride=chips), :] = block[:, i * LANES : (i + 1) * LANES]

    def token(t, _):
        here = pl.ds(pl.multiple_of(t * chips, chips), chips)
        row = jnp.concatenate([ref[here, :] for ref in lanes], axis=1).astype(jnp.bfloat16)
        for k in range(topk):
            e = index_ref[k, t]
            rank = count_ref[e]
            count_ref[e] = rank + 1
            out_ref[e, rank] = row

    lax.fori_loop(0, tokens, token, None)


def fetch_kernel(
    gate_hbm, up_hbm, down_hbm, near_ref, far_hbm, cross_hbm, near_sems, far_sems, cross_sems
):
    core = lax.axis_index("tp") % 2
    copies = into_blocks(gate_hbm, up_hbm, 1 - core, far_hbm, far_sems)
    copies += columns(down_hbm, 1 - core, cross_hbm, cross_sems)
    copies += into_blocks(gate_hbm, up_hbm, core, near_ref, near_sems)
    for copy in copies:
        copy.start()
    for copy in copies:
        copy.wait()


def sums_kernel(x_ref, near_ref, far_ref, sums_ref, *lanes):
    slots, chips, share = x_ref.shape
    for i, ref in enumerate(lanes):
        part = x_ref[:, :, i * LANES : (i + 1) * LANES].astype(jnp.float32)
        ref[...] = part.reshape(slots * chips, LANES)
    sums = [jnp.zeros(sums_ref.shape[1:], jnp.float32)] * 4
    for b in range(chips):
        rows = pl.ds(b, slots, stride=chips)
        x = jnp.concatenate([ref[rows, :] for ref in lanes], axis=1).astype(jnp.bfloat16)
        for i in range(4):
            w = (near_ref, far_ref)[i // 2][i % 2, b]
            sums[i] += jnp.dot(x, w, preferred_element_type=jnp.float32)
    for i in range(4):
        sums_ref[i] = sums[i]


def down_kernel(down_hbm, crossed_hbm, out_ref, sems, sem):
    units = down_hbm.shape[0]
    copies = columns(down_hbm, lax.axis_index("tp") % 2, out_ref.at[:units], sems)
    copies.append(pltpu.make_async_copy(crossed_hbm, out_ref.at[units:], sem))
    for copy in copies:
        copy.start()
    for copy in copies:
        copy.wait()


def output_kernel(own_ref, theirs_ref, down_ref, out_ref, *lanes):
    slots, chips, share = out_ref.shape
    hidden = []
    for i in (0, 2):
        gate = own_ref[i] + theirs_ref[2 - i]
        up = own_ref[i + 1] + theirs_ref[3 - i]
        hidden.append((gate * jax.nn.sigmoid(gate) * up).astype(jnp.bfloat16))
    hidden = jnp.concatenate(hidden, axis=1)
    for b in range(chips):
        at = pl.ds(b * BLOCK, BLOCK)
        out = jnp.dot(hidden, down_ref[:, at], preferred_element_type=jnp.float32)
        for i, ref in enumerate(lanes):
            ref[pl.ds(b, slots, stride=chips), :] = out[:, i * LANES : (i + 1) * LANES]
    for i, ref in enumerate(lanes):
        part = ref[...].reshape(slots, chips, LANES).astype(jnp.bfloat16)
        out_ref[:, :, i * LANES : (i + 1) * LANES] = part


GRANT = pltpu.CompilerParams(vmem_limit_bytes=16 * 2**20)
VMEM = pl.BlockSpec(memory_space=pltpu.VMEM)
HBM = pl.BlockSpec(memory_space=pltpu.HBM)


def in_vmem(x):
    return pltpu.with_memory_space_constraint(x, pltpu.VMEM)


def in_hbm(x):
    return pltpu.with_memory_space_constraint(x, pltpu.HBM)


def body(tokens, norm_gain, token_expert_index, group_prob, expert_weight, w_gate, w_up, w_down):
    rows_here, width = tokens.shape
    topk = token_expert_index.shape[1]
    experts = lax.axis_size("ep")
    tp_count = lax.axis_size("tp")
    chips = tp_count // 2
    share = width // tp_count
    half = width // 2
    units = w_gate.shape[2]
    swap = [(i, i ^ 1) for i in range(tp_count)]
    same_core = [[2 * i + c for i in range(chips)] for c in range(2)]
    per_group = experts // GROUPS
    capacity = min(rows_here, max(2, rows_here * topk // max(per_group - topk, 1) + 1))
    slots_total = experts * capacity
    gates = group_prob[:, None] * expert_weight / jnp.sum(expert_weight, axis=-1, keepdims=True)
    flattened_index = token_expert_index.reshape(-1)
    onehot = (flattened_index[:, None] == jnp.arange(experts, dtype=jnp.int32)[None, :]).astype(
        jnp.int32
    )
    earlier = jnp.cumsum(onehot, axis=0) - onehot
    slot_rank = jnp.sum(earlier * onehot, axis=1)
    place = flattened_index * capacity + slot_rank
    at_place = jnp.arange(slots_total, dtype=jnp.int32)[:, None] == place[None, :]

    weigh = jnp.sum(
        (at_place.astype(jnp.float32) * gates.reshape(-1)[None, :]).reshape(
            slots_total, rows_here, topk
        ),
        axis=2,
    )

    weights = [in_hbm(w[0]) for w in (w_gate, w_up, w_down)]
    lanes = [pltpu.VMEM((slots_total * chips, LANES), jnp.float32)] * (share // LANES)
    outgoing = pl.pallas_call(
        dispatch_kernel,
        out_shape=jax.ShapeDtypeStruct((experts, capacity, chips, share), jnp.bfloat16),
        in_specs=[HBM, HBM, HBM],
        out_specs=VMEM,
        scratch_shapes=[
            pltpu.SMEM((topk, rows_here), jnp.int32),
            pltpu.VMEM((rows_here, width), jnp.bfloat16),
            pltpu.VMEM((1, width), jnp.float32),
            pltpu.SMEM((experts,), jnp.int32),
            pltpu.SemaphoreType.DMA((3,)),
            *[pltpu.VMEM((rows_here * chips, LANES), jnp.float32)] * (share // LANES),
        ],
        compiler_params=GRANT,
        name="dispatch",
    )(*(in_hbm(x) for x in (token_expert_index.T, tokens, norm_gain[None, :])))
    outgoing = outgoing.reshape(experts, capacity * chips, share)
    near, far, cross = pl.pallas_call(
        fetch_kernel,
        out_shape=(
            pltpu.VMEM((2, chips, share, units), jnp.bfloat16),
            pltpu.HBM((2, chips, share, units), jnp.bfloat16),
            pltpu.HBM((units, half), jnp.bfloat16),
        ),
        in_specs=[HBM, HBM, HBM],
        out_specs=(VMEM, HBM, HBM),
        scratch_shapes=[
            pltpu.SemaphoreType.DMA((2, chips)),
            pltpu.SemaphoreType.DMA((2, chips)),
            pltpu.SemaphoreType.DMA((chips,)),
        ],
        compiler_params=GRANT,
        name="fetch",
    )(*weights)
    far = lax.ppermute(far, "tp", swap)
    cross = lax.ppermute(cross, "tp", swap)
    arrived = lax.all_to_all(outgoing, "ep", split_axis=0, concat_axis=0, tiled=True)
    arrived, near, far, cross, weigh = lax.optimization_barrier((arrived, near, far, cross, weigh))
    sums = pl.pallas_call(
        sums_kernel,
        out_shape=pltpu.VMEM((4, slots_total, units), jnp.float32),
        in_specs=[VMEM, VMEM, VMEM],
        out_specs=VMEM,
        scratch_shapes=lanes,
        compiler_params=GRANT,
        name="sums",
    )(*(in_vmem(x) for x in (arrived.reshape(slots_total, chips, share), near, far)))
    theirs = lax.ppermute(sums, "tp", swap)
    down = pl.pallas_call(
        down_kernel,
        out_shape=pltpu.VMEM((2 * units, half), jnp.bfloat16),
        in_specs=[HBM, HBM],
        out_specs=VMEM,
        scratch_shapes=[pltpu.SemaphoreType.DMA((chips,)), pltpu.SemaphoreType.DMA],
        compiler_params=GRANT,
        name="down",
    )(weights[2], in_hbm(cross))
    mine = pl.pallas_call(
        output_kernel,
        out_shape=pltpu.VMEM((slots_total, chips, share), jnp.bfloat16),
        in_specs=[VMEM, VMEM, VMEM],
        out_specs=VMEM,
        scratch_shapes=lanes,
        compiler_params=GRANT,
        name="output",
    )(*(in_vmem(x) for x in (sums, theirs, down)))
    mine = mine.reshape(experts, capacity * chips, share)
    returned = lax.all_to_all(mine, "ep", split_axis=0, concat_axis=0, tiled=True)
    returned = returned.reshape(slots_total, half)
    partial_mix = jnp.dot(
        weigh.T,
        returned.astype(jnp.float32),
        precision=lax.Precision.HIGHEST,
        preferred_element_type=jnp.float32,
    ).astype(jnp.bfloat16)
    blocks = jnp.moveaxis(partial_mix.reshape(rows_here, chips, share), 1, 0)
    parts = lax.all_to_all(
        blocks, "tp", split_axis=0, concat_axis=0, tiled=True, axis_index_groups=same_core
    )
    return parts.astype(jnp.float32).sum(axis=0).astype(jnp.bfloat16)


def solution(mesh):
    return jax.shard_map(
        body,
        mesh=mesh,
        in_specs=(
            P("ep", None),
            P(),
            P("ep", None),
            P("ep"),
            P("ep", None),
            P("ep", None, "tp"),
            P("ep", None, "tp"),
            P("ep", "tp", None),
        ),
        out_specs=P("ep", "tp"),
        check_vma=False,
    )
```

```python
import jax
import jax.numpy as jnp
from jax import lax
from jax.experimental import pallas as pl
from jax.experimental.pallas import tpu as pltpu
from jax.sharding import PartitionSpec as P

GROUPS = 2
BLOCK = 256
LANES = 128


def block_at(b, which):
    return pl.ds(pl.multiple_of((2 * b + which) * BLOCK, BLOCK), BLOCK)


def into_blocks(gate_hbm, up_hbm, which, out_ref, sems):
    return [
        pltpu.make_async_copy(hbm.at[block_at(b, which)], out_ref.at[i, b], sems.at[i, b])
        for b in range(out_ref.shape[1])
        for i, hbm in enumerate((gate_hbm, up_hbm))
    ]


def columns(hbm, which, out_ref, sems):
    return [
        pltpu.make_async_copy(
            hbm.at[:, block_at(b, which)], out_ref.at[:, b * BLOCK : (b + 1) * BLOCK], sems.at[b]
        )
        for b in range(out_ref.shape[1] // BLOCK)
    ]


def dispatch_kernel(
    index_hbm, tokens_hbm, gain_hbm,
    out_ref,
    index_ref, tokens_ref, gain_ref, count_ref, sems, *lanes,
):
    core = lax.axis_index("tp") % 2
    tokens, width = tokens_ref.shape
    experts, _, chips, share = out_ref.shape
    topk = index_ref.shape[0]
    copies = [
        pltpu.make_async_copy(hbm, ref, sems.at[i])
        for i, (hbm, ref) in enumerate(
            ((tokens_hbm, tokens_ref), (index_hbm, index_ref), (gain_hbm, gain_ref))
        )
    ]
    for copy in copies:
        copy.start()
    out_ref[...] = jnp.zeros_like(out_ref)

    def clear(e, _):
        count_ref[e] = 0

    lax.fori_loop(0, experts, clear, None, unroll=8)
    for copy in copies:
        copy.wait()
    xf = tokens_ref[...].astype(jnp.float32)
    scale = lax.rsqrt(jnp.mean(xf * xf, axis=-1, keepdims=True) + 1e-06)
    for b in range(chips):
        at = block_at(b, core)
        block = tokens_ref[:, at].astype(jnp.float32) * scale * gain_ref[:, at]
        for i, ref in enumerate(lanes):
            ref[pl.ds(b, tokens, stride=chips), :] = block[:, i * LANES : (i + 1) * LANES]

    def token(t, _):
        here = pl.ds(pl.multiple_of(t * chips, chips), chips)
        row = jnp.concatenate([ref[here, :] for ref in lanes], axis=1).astype(jnp.bfloat16)
        for k in range(topk):
            e = index_ref[k, t]
            rank = count_ref[e]
            count_ref[e] = rank + 1
            out_ref[e, rank] = row

    lax.fori_loop(0, tokens, token, None)


def fetch_kernel(
    gate_hbm, up_hbm, down_hbm, near_ref, far_ref, cross_ref, near_sems, far_sems, cross_sems
):
    core = lax.axis_index("tp") % 2
    copies = into_blocks(gate_hbm, up_hbm, 1 - core, far_ref, far_sems)
    copies += columns(down_hbm, 1 - core, cross_ref, cross_sems)
    copies += into_blocks(gate_hbm, up_hbm, core, near_ref, near_sems)
    for copy in copies:
        copy.start()
    for copy in copies:
        copy.wait()


def sums_kernel(x_ref, near_ref, far_ref, sums_ref, *lanes):
    slots, chips, share = x_ref.shape
    for i, ref in enumerate(lanes):
        part = x_ref[:, :, i * LANES : (i + 1) * LANES].astype(jnp.float32)
        ref[...] = part.reshape(slots * chips, LANES)
    sums = [jnp.zeros(sums_ref.shape[1:], jnp.float32)] * 4
    for b in range(chips):
        rows = pl.ds(b, slots, stride=chips)
        x = jnp.concatenate([ref[rows, :] for ref in lanes], axis=1).astype(jnp.bfloat16)
        for i in range(4):
            w = (near_ref, far_ref)[i // 2][i % 2, b]
            sums[i] += jnp.dot(x, w, preferred_element_type=jnp.float32)
    for i in range(4):
        sums_ref[i] = sums[i]


def down_kernel(down_hbm, crossed_hbm, out_ref, sems, sem):
    units = down_hbm.shape[0]
    copies = columns(down_hbm, lax.axis_index("tp") % 2, out_ref.at[:units], sems)
    copies.append(pltpu.make_async_copy(crossed_hbm, out_ref.at[units:], sem))
    for copy in copies:
        copy.start()
    for copy in copies:
        copy.wait()


def output_kernel(own_ref, theirs_ref, down_ref, out_ref, *lanes):
    slots, chips, share = out_ref.shape
    hidden = []
    for i in (0, 2):
        gate = own_ref[i] + theirs_ref[2 - i]
        up = own_ref[i + 1] + theirs_ref[3 - i]
        hidden.append((gate * jax.nn.sigmoid(gate) * up).astype(jnp.bfloat16))
    hidden = jnp.concatenate(hidden, axis=1)
    for b in range(chips):
        at = pl.ds(b * BLOCK, BLOCK)
        out = jnp.dot(hidden, down_ref[:, at], preferred_element_type=jnp.float32)
        for i, ref in enumerate(lanes):
            ref[pl.ds(b, slots, stride=chips), :] = out[:, i * LANES : (i + 1) * LANES]
    for i, ref in enumerate(lanes):
        part = ref[...].reshape(slots, chips, LANES).astype(jnp.bfloat16)
        out_ref[:, :, i * LANES : (i + 1) * LANES] = part


GRANT = pltpu.CompilerParams(vmem_limit_bytes=16 * 2**20)
VMEM = pl.BlockSpec(memory_space=pltpu.VMEM)
HBM = pl.BlockSpec(memory_space=pltpu.HBM)


def in_vmem(x):
    return pltpu.with_memory_space_constraint(x, pltpu.VMEM)


def in_hbm(x):
    return pltpu.with_memory_space_constraint(x, pltpu.HBM)


def body(tokens, norm_gain, token_expert_index, group_prob, expert_weight, w_gate, w_up, w_down):
    rows_here, width = tokens.shape
    topk = token_expert_index.shape[1]
    experts = lax.axis_size("ep")
    tp_count = lax.axis_size("tp")
    chips = tp_count // 2
    share = width // tp_count
    half = width // 2
    units = w_gate.shape[2]
    swap = [(i, i ^ 1) for i in range(tp_count)]
    same_core = [[2 * i + c for i in range(chips)] for c in range(2)]
    per_group = experts // GROUPS
    capacity = min(rows_here, max(2, rows_here * topk // max(per_group - topk, 1) + 1))
    slots_total = experts * capacity
    gates = group_prob[:, None] * expert_weight / jnp.sum(expert_weight, axis=-1, keepdims=True)
    flattened_index = token_expert_index.reshape(-1)
    onehot = (flattened_index[:, None] == jnp.arange(experts, dtype=jnp.int32)[None, :]).astype(
        jnp.int32
    )
    earlier = jnp.cumsum(onehot, axis=0) - onehot
    slot_rank = jnp.sum(earlier * onehot, axis=1)
    place = flattened_index * capacity + slot_rank
    at_place = jnp.arange(slots_total, dtype=jnp.int32)[:, None] == place[None, :]

    weigh = jnp.sum(
        (at_place.astype(jnp.float32) * gates.reshape(-1)[None, :]).reshape(
            slots_total, rows_here, topk
        ),
        axis=2,
    )

    weights = [in_hbm(w[0]) for w in (w_gate, w_up, w_down)]
    lanes = [pltpu.VMEM((slots_total * chips, LANES), jnp.float32)] * (share // LANES)
    outgoing = pl.pallas_call(
        dispatch_kernel,
        out_shape=jax.ShapeDtypeStruct((experts, capacity, chips, share), jnp.bfloat16),
        in_specs=[HBM, HBM, HBM],
        out_specs=VMEM,
        scratch_shapes=[
            pltpu.SMEM((topk, rows_here), jnp.int32),
            pltpu.VMEM((rows_here, width), jnp.bfloat16),
            pltpu.VMEM((1, width), jnp.float32),
            pltpu.SMEM((experts,), jnp.int32),
            pltpu.SemaphoreType.DMA((3,)),
            *[pltpu.VMEM((rows_here * chips, LANES), jnp.float32)] * (share // LANES),
        ],
        compiler_params=GRANT,
        name="dispatch",
    )(*(in_hbm(x) for x in (token_expert_index.T, tokens, norm_gain[None, :])))
    outgoing = outgoing.reshape(experts, capacity * chips, share)
    near, far, cross = pl.pallas_call(
        fetch_kernel,
        out_shape=(
            pltpu.VMEM((2, chips, share, units), jnp.bfloat16),
            jax.ShapeDtypeStruct((2, chips, share, units), jnp.bfloat16),
            jax.ShapeDtypeStruct((units, half), jnp.bfloat16),
        ),
        in_specs=[HBM, HBM, HBM],
        out_specs=(VMEM, VMEM, VMEM),
        scratch_shapes=[
            pltpu.SemaphoreType.DMA((2, chips)),
            pltpu.SemaphoreType.DMA((2, chips)),
            pltpu.SemaphoreType.DMA((chips,)),
        ],
        compiler_params=GRANT,
        name="fetch",
    )(*weights)
    far = lax.ppermute(far, "tp", swap)
    cross = lax.ppermute(cross, "tp", swap)
    arrived = lax.all_to_all(outgoing, "ep", split_axis=0, concat_axis=0, tiled=True)
    arrived, near, far, cross, weigh = lax.optimization_barrier((arrived, near, far, cross, weigh))
    sums = pl.pallas_call(
        sums_kernel,
        out_shape=pltpu.VMEM((4, slots_total, units), jnp.float32),
        in_specs=[VMEM, VMEM, VMEM],
        out_specs=VMEM,
        scratch_shapes=lanes,
        compiler_params=GRANT,
        name="sums",
    )(*(in_vmem(x) for x in (arrived.reshape(slots_total, chips, share), near, far)))
    theirs = lax.ppermute(sums, "tp", swap)
    down = pl.pallas_call(
        down_kernel,
        out_shape=pltpu.VMEM((2 * units, half), jnp.bfloat16),
        in_specs=[HBM, HBM],
        out_specs=VMEM,
        scratch_shapes=[pltpu.SemaphoreType.DMA((chips,)), pltpu.SemaphoreType.DMA],
        compiler_params=GRANT,
        name="down",
    )(weights[2], in_hbm(cross))
    mine = pl.pallas_call(
        output_kernel,
        out_shape=pltpu.VMEM((slots_total, chips, share), jnp.bfloat16),
        in_specs=[VMEM, VMEM, VMEM],
        out_specs=VMEM,
        scratch_shapes=lanes,
        compiler_params=GRANT,
        name="output",
    )(*(in_vmem(x) for x in (sums, theirs, down)))
    mine = mine.reshape(experts, capacity * chips, share)
    returned = lax.all_to_all(mine, "ep", split_axis=0, concat_axis=0, tiled=True)
    returned = returned.reshape(slots_total, half)
    partial_mix = jnp.dot(
        weigh.T,
        returned.astype(jnp.float32),
        precision=lax.Precision.HIGHEST,
        preferred_element_type=jnp.float32,
    ).astype(jnp.bfloat16)
    blocks = jnp.moveaxis(partial_mix.reshape(rows_here, chips, share), 1, 0)
    parts = lax.all_to_all(
        blocks, "tp", split_axis=0, concat_axis=0, tiled=True, axis_index_groups=same_core
    )
    return parts.astype(jnp.float32).sum(axis=0).astype(jnp.bfloat16)


def solution(mesh):
    return jax.shard_map(
        body,
        mesh=mesh,
        in_specs=(
            P("ep", None),
            P(),
            P("ep", None),
            P("ep"),
            P("ep", None),
            P("ep", None, "tp"),
            P("ep", None, "tp"),
            P("ep", "tp", None),
        ),
        out_specs=P("ep", "tp"),
        check_vma=False,
    )
```

```python
import jax
import jax.numpy as jnp
from jax import lax
from jax.experimental import pallas as pl
from jax.experimental.pallas import tpu as pltpu
from jax.sharding import PartitionSpec as P

GROUPS = 2
BLOCK = 256
LANES = 128


def block_at(b, which):
    return pl.ds(pl.multiple_of((2 * b + which) * BLOCK, BLOCK), BLOCK)


def into_blocks(gate_hbm, up_hbm, which, out_ref, sems):
    return [
        pltpu.make_async_copy(hbm.at[block_at(b, which)], out_ref.at[i, b], sems.at[i, b])
        for b in range(out_ref.shape[1])
        for i, hbm in enumerate((gate_hbm, up_hbm))
    ]


def columns(hbm, which, out_ref, sems):
    return [
        pltpu.make_async_copy(
            hbm.at[:, pl.ds(pl.multiple_of((4 * b + which) * BLOCK, BLOCK), BLOCK)],
            out_ref.at[:, b * BLOCK : (b + 1) * BLOCK],
            sems.at[b],
        )
        for b in range(out_ref.shape[1] // BLOCK)
    ]


def beside(d):
    here = lax.axis_index("tp") % 4
    flipped = here + 1 - 2 * (here % 2) if d % 2 else here
    return (flipped + 2) % 4 if d > 1 else flipped


def dispatch_kernel(
    index_hbm, tokens_hbm, gain_hbm,
    out_ref,
    index_ref, tokens_ref, gain_ref, count_ref, sems, *lanes,
):
    core = lax.axis_index("tp") % 2
    tokens, width = tokens_ref.shape
    experts, _, chips, share = out_ref.shape
    topk = index_ref.shape[0]
    copies = [
        pltpu.make_async_copy(hbm, ref, sems.at[i])
        for i, (hbm, ref) in enumerate(
            ((tokens_hbm, tokens_ref), (index_hbm, index_ref), (gain_hbm, gain_ref))
        )
    ]
    for copy in copies:
        copy.start()
    out_ref[...] = jnp.zeros_like(out_ref)

    def clear(e, _):
        count_ref[e] = 0

    lax.fori_loop(0, experts, clear, None, unroll=8)
    for copy in copies:
        copy.wait()
    xf = tokens_ref[...].astype(jnp.float32)
    scale = lax.rsqrt(jnp.mean(xf * xf, axis=-1, keepdims=True) + 1e-06)
    for b in range(chips):
        at = block_at(b, core)
        block = tokens_ref[:, at].astype(jnp.float32) * scale * gain_ref[:, at]
        for i, ref in enumerate(lanes):
            ref[pl.ds(b, tokens, stride=chips), :] = block[:, i * LANES : (i + 1) * LANES]

    def token(t, _):
        here = pl.ds(pl.multiple_of(t * chips, chips), chips)
        row = jnp.concatenate([ref[here, :] for ref in lanes], axis=1).astype(jnp.bfloat16)
        for k in range(topk):
            e = index_ref[k, t]
            rank = count_ref[e]
            count_ref[e] = rank + 1
            out_ref[e, rank] = row

    lax.fori_loop(0, tokens, token, None)


def fetch_kernel(
    gate_hbm, up_hbm, down_hbm, near_ref, far_ref, *refs
):
    core = lax.axis_index("tp") % 2
    crosses, (near_sems, far_sems, cross_sems) = refs[:3], refs[3:]
    copies = into_blocks(gate_hbm, up_hbm, 1 - core, far_ref, far_sems)
    for i, ref in enumerate(crosses):
        copies += columns(down_hbm, beside(i + 1), ref, cross_sems.at[i])
    copies += into_blocks(gate_hbm, up_hbm, core, near_ref, near_sems)
    for copy in copies:
        copy.start()
    for copy in copies:
        copy.wait()


def sums_kernel(x_ref, near_ref, far_ref, sums_ref, *lanes):
    slots, chips, share = x_ref.shape
    for i, ref in enumerate(lanes):
        part = x_ref[:, :, i * LANES : (i + 1) * LANES].astype(jnp.float32)
        ref[...] = part.reshape(slots * chips, LANES)
    sums = [jnp.zeros(sums_ref.shape[1:], jnp.float32)] * 4
    for b in range(chips):
        rows = pl.ds(b, slots, stride=chips)
        x = jnp.concatenate([ref[rows, :] for ref in lanes], axis=1).astype(jnp.bfloat16)
        for i in range(4):
            w = (near_ref, far_ref)[i // 2][i % 2, b]
            sums[i] += jnp.dot(x, w, preferred_element_type=jnp.float32)
    for i in range(4):
        sums_ref[i] = sums[i]


def down_kernel(down_hbm, *refs):
    crossed, (out_ref, sems, crossed_sems) = refs[:3], refs[3:]
    units = down_hbm.shape[0]
    copies = columns(down_hbm, beside(0), out_ref.at[:units], sems)
    for i, hbm in enumerate(crossed):
        there = out_ref.at[(i + 1) * units : (i + 2) * units]
        copies.append(pltpu.make_async_copy(hbm, there, crossed_sems.at[i]))
    for copy in copies:
        copy.start()
    for copy in copies:
        copy.wait()


def hidden_kernel(own_ref, theirs_ref, out_ref):
    hidden = []
    for i in (0, 2):
        gate = own_ref[i] + theirs_ref[2 - i]
        up = own_ref[i + 1] + theirs_ref[3 - i]
        hidden.append((gate * jax.nn.sigmoid(gate) * up).astype(jnp.bfloat16))
    out_ref[...] = jnp.concatenate(hidden, axis=1)


def output_kernel(own_ref, theirs_ref, down_ref, out_ref, rows_ref):
    slots, rows, _ = out_ref.shape
    hidden = jnp.concatenate([own_ref[...], theirs_ref[...]], axis=1)
    parts = BLOCK // LANES
    for b in range(rows // parts):
        at = pl.ds(b * BLOCK, BLOCK)
        out = jnp.dot(hidden, down_ref[:, at], preferred_element_type=jnp.float32)
        for i in range(parts):
            row = pl.ds(b * parts + i, slots, stride=rows)
            rows_ref[row, :] = out[:, i * LANES : (i + 1) * LANES]
    out_ref[...] = rows_ref[...].reshape(out_ref.shape).astype(jnp.bfloat16)


GRANT = pltpu.CompilerParams(vmem_limit_bytes=16 * 2**20)
VMEM = pl.BlockSpec(memory_space=pltpu.VMEM)
HBM = pl.BlockSpec(memory_space=pltpu.HBM)


def in_vmem(x):
    return pltpu.with_memory_space_constraint(x, pltpu.VMEM)


def in_hbm(x):
    return pltpu.with_memory_space_constraint(x, pltpu.HBM)


def body(tokens, norm_gain, token_expert_index, group_prob, expert_weight, w_gate, w_up, w_down):
    rows_here, width = tokens.shape
    topk = token_expert_index.shape[1]
    experts = lax.axis_size("ep")
    tp_count = lax.axis_size("tp")
    chips = tp_count // 2
    share = width // tp_count
    half = width // 2
    units = w_gate.shape[2]
    swap = [(i, i ^ 1) for i in range(tp_count)]
    across = [[(i, i ^ d) for i in range(tp_count)] for d in (1, 2, 3)]
    quarter = width // 4
    every_fourth = [[4 * j + q for j in range(tp_count // 4)] for q in range(4)]
    per_group = experts // GROUPS
    capacity = min(rows_here, max(2, rows_here * topk // max(per_group - topk, 1) + 1))
    slots_total = experts * capacity
    gates = group_prob[:, None] * expert_weight / jnp.sum(expert_weight, axis=-1, keepdims=True)
    flattened_index = token_expert_index.reshape(-1)
    onehot = (flattened_index[:, None] == jnp.arange(experts, dtype=jnp.int32)[None, :]).astype(
        jnp.int32
    )
    earlier = jnp.cumsum(onehot, axis=0) - onehot
    slot_rank = jnp.sum(earlier * onehot, axis=1)
    place = flattened_index * capacity + slot_rank
    at_place = jnp.arange(slots_total, dtype=jnp.int32)[:, None] == place[None, :]

    weigh = jnp.sum(
        (at_place.astype(jnp.float32) * gates.reshape(-1)[None, :]).reshape(
            slots_total, rows_here, topk
        ),
        axis=2,
    )

    weights = [in_hbm(w[0]) for w in (w_gate, w_up, w_down)]
    lanes = [pltpu.VMEM((slots_total * chips, LANES), jnp.float32)] * (share // LANES)
    outgoing = pl.pallas_call(
        dispatch_kernel,
        out_shape=jax.ShapeDtypeStruct((experts, capacity, chips, share), jnp.bfloat16),
        in_specs=[HBM, HBM, HBM],
        out_specs=VMEM,
        scratch_shapes=[
            pltpu.SMEM((topk, rows_here), jnp.int32),
            pltpu.VMEM((rows_here, width), jnp.bfloat16),
            pltpu.VMEM((1, width), jnp.float32),
            pltpu.SMEM((experts,), jnp.int32),
            pltpu.SemaphoreType.DMA((3,)),
            *[pltpu.VMEM((rows_here * chips, LANES), jnp.float32)] * (share // LANES),
        ],
        compiler_params=GRANT,
        name="dispatch",
    )(*(in_hbm(x) for x in (token_expert_index.T, tokens, norm_gain[None, :])))
    outgoing = outgoing.reshape(experts, capacity * chips, share)
    near, far, *crosses = pl.pallas_call(
        fetch_kernel,
        out_shape=(
            pltpu.VMEM((2, chips, share, units), jnp.bfloat16),
            jax.ShapeDtypeStruct((2, chips, share, units), jnp.bfloat16),
            *[jax.ShapeDtypeStruct((units, quarter), jnp.bfloat16)] * 3,
        ),
        in_specs=[HBM, HBM, HBM],
        out_specs=(VMEM,) * 5,
        scratch_shapes=[
            pltpu.SemaphoreType.DMA((2, chips)),
            pltpu.SemaphoreType.DMA((2, chips)),
            pltpu.SemaphoreType.DMA((3, quarter // BLOCK)),
        ],
        compiler_params=GRANT,
        name="fetch",
    )(*weights)
    far = lax.ppermute(far, "tp", swap)
    crosses = [lax.ppermute(x, "tp", to) for x, to in zip(crosses, across)]
    arrived = lax.all_to_all(outgoing, "ep", split_axis=0, concat_axis=0, tiled=True)
    arrived, near, far, crosses, weigh = lax.optimization_barrier(
        (arrived, near, far, crosses, weigh)
    )
    sums = pl.pallas_call(
        sums_kernel,
        out_shape=pltpu.VMEM((4, slots_total, units), jnp.float32),
        in_specs=[VMEM, VMEM, VMEM],
        out_specs=VMEM,
        scratch_shapes=lanes,
        compiler_params=GRANT,
        name="sums",
    )(*(in_vmem(x) for x in (arrived.reshape(slots_total, chips, share), near, far)))
    theirs = lax.ppermute(sums, "tp", swap)
    down = pl.pallas_call(
        down_kernel,
        out_shape=pltpu.VMEM((4 * units, quarter), jnp.bfloat16),
        in_specs=[HBM] * 4,
        out_specs=VMEM,
        scratch_shapes=[
            pltpu.SemaphoreType.DMA((quarter // BLOCK,)),
            pltpu.SemaphoreType.DMA((3,)),
        ],
        compiler_params=GRANT,
        name="down",
    )(weights[2], *(in_hbm(x) for x in crosses))
    hidden = pl.pallas_call(
        hidden_kernel,
        out_shape=pltpu.VMEM((slots_total, 2 * units), jnp.bfloat16),
        in_specs=[VMEM, VMEM],
        out_specs=VMEM,
        compiler_params=GRANT,
        name="hidden",
    )(in_vmem(sums), in_vmem(theirs))
    beyond = lax.ppermute(hidden, "tp", across[1])
    rows = quarter // LANES
    mine = pl.pallas_call(
        output_kernel,
        out_shape=pltpu.VMEM((slots_total, rows, LANES), jnp.bfloat16),
        in_specs=[VMEM, VMEM, VMEM],
        out_specs=VMEM,
        scratch_shapes=[pltpu.VMEM((slots_total * rows, LANES), jnp.float32)],
        compiler_params=GRANT,
        name="output",
    )(*(in_vmem(x) for x in (hidden, beyond, down)))
    mine = mine.reshape(experts, capacity * rows, LANES)
    returned = lax.all_to_all(mine, "ep", split_axis=0, concat_axis=0, tiled=True)
    returned = returned.reshape(slots_total, quarter)
    partial_mix = jnp.dot(
        weigh.T,
        returned.astype(jnp.float32),
        precision=lax.Precision.HIGHEST,
        preferred_element_type=jnp.float32,
    ).astype(jnp.bfloat16)
    blocks = jnp.moveaxis(partial_mix.reshape(rows_here, quarter // share, share), 1, 0)
    parts = lax.all_to_all(
        blocks, "tp", split_axis=0, concat_axis=0, tiled=True, axis_index_groups=every_fourth
    )
    return parts.astype(jnp.float32).sum(axis=0).astype(jnp.bfloat16)


def solution(mesh):
    return jax.shard_map(
        body,
        mesh=mesh,
        in_specs=(
            P("ep", None),
            P(),
            P("ep", None),
            P("ep"),
            P("ep", None),
            P("ep", None, "tp"),
            P("ep", None, "tp"),
            P("ep", "tp", None),
        ),
        out_specs=P("ep", "tp"),
        check_vma=False,
    )
```

```python
import jax
import jax.numpy as jnp
from jax import lax
from jax.experimental import pallas as pl
from jax.experimental.pallas import tpu as pltpu
from jax.sharding import PartitionSpec as P

GROUPS = 2
BLOCK = 256
LANES = 128


def block_at(b, which):
    return pl.ds(pl.multiple_of((2 * b + which) * BLOCK, BLOCK), BLOCK)


def into_blocks(gate_hbm, up_hbm, which, out_ref, sems):
    return [
        pltpu.make_async_copy(hbm.at[block_at(b, which)], out_ref.at[i, b], sems.at[i, b])
        for b in range(out_ref.shape[1])
        for i, hbm in enumerate((gate_hbm, up_hbm))
    ]


def columns(hbm, which, out_ref, sems):
    return [
        pltpu.make_async_copy(
            hbm.at[:, block_at(b, which)], out_ref.at[:, b * BLOCK : (b + 1) * BLOCK], sems.at[b]
        )
        for b in range(out_ref.shape[1] // BLOCK)
    ]


def dispatch_kernel(
    index_hbm, tokens_hbm, gain_hbm,
    out_ref,
    index_ref, tokens_ref, gain_ref, count_ref, sems, *lanes,
):
    core = lax.axis_index("tp") % 2
    tokens, width = tokens_ref.shape
    experts, _, chips, share = out_ref.shape
    topk = index_ref.shape[0]
    copies = [
        pltpu.make_async_copy(hbm, ref, sems.at[i])
        for i, (hbm, ref) in enumerate(
            ((tokens_hbm, tokens_ref), (index_hbm, index_ref), (gain_hbm, gain_ref))
        )
    ]
    for copy in copies:
        copy.start()
    out_ref[...] = jnp.zeros_like(out_ref)

    def clear(e, _):
        count_ref[e] = 0

    lax.fori_loop(0, experts, clear, None, unroll=8)
    for copy in copies:
        copy.wait()
    xf = tokens_ref[...].astype(jnp.float32)
    scale = lax.rsqrt(jnp.mean(xf * xf, axis=-1, keepdims=True) + 1e-06)
    for b in range(chips):
        at = block_at(b, core)
        block = tokens_ref[:, at].astype(jnp.float32) * scale * gain_ref[:, at]
        for i, ref in enumerate(lanes):
            ref[pl.ds(b, tokens, stride=chips), :] = block[:, i * LANES : (i + 1) * LANES]

    def token(t, _):
        here = pl.ds(pl.multiple_of(t * chips, chips), chips)
        row = jnp.concatenate([ref[here, :] for ref in lanes], axis=1).astype(jnp.bfloat16)
        for k in range(topk):
            e = index_ref[k, t]
            rank = count_ref[e]
            count_ref[e] = rank + 1
            out_ref[e, rank] = row

    lax.fori_loop(0, tokens, token, None, unroll=True)


def fetch_kernel(
    gate_hbm, up_hbm, down_hbm, near_ref, far_ref, cross_ref, near_sems, far_sems, cross_sems
):
    core = lax.axis_index("tp") % 2
    copies = into_blocks(gate_hbm, up_hbm, 1 - core, far_ref, far_sems)
    copies += columns(down_hbm, 1 - core, cross_ref, cross_sems)
    copies += into_blocks(gate_hbm, up_hbm, core, near_ref, near_sems)
    for copy in copies:
        copy.start()
    for copy in copies:
        copy.wait()


def sums_kernel(x_ref, near_ref, far_ref, sums_ref, *lanes):
    slots, chips, share = x_ref.shape
    for i, ref in enumerate(lanes):
        part = x_ref[:, :, i * LANES : (i + 1) * LANES].astype(jnp.float32)
        ref[...] = part.reshape(slots * chips, LANES)
    sums = [jnp.zeros(sums_ref.shape[1:], jnp.float32)] * 4
    for b in range(chips):
        rows = pl.ds(b, slots, stride=chips)
        x = jnp.concatenate([ref[rows, :] for ref in lanes], axis=1).astype(jnp.bfloat16)
        for i in range(4):
            w = (near_ref, far_ref)[i // 2][i % 2, b]
            sums[i] += jnp.dot(x, w, preferred_element_type=jnp.float32)
    for i in range(4):
        sums_ref[i] = sums[i]


def down_kernel(down_hbm, crossed_hbm, out_ref, sems, sem):
    units = down_hbm.shape[0]
    copies = columns(down_hbm, lax.axis_index("tp") % 2, out_ref.at[:units], sems)
    copies.append(pltpu.make_async_copy(crossed_hbm, out_ref.at[units:], sem))
    for copy in copies:
        copy.start()
    for copy in copies:
        copy.wait()


def output_kernel(own_ref, theirs_ref, down_ref, out_ref, rows_ref):
    slots, rows, _ = out_ref.shape
    hidden = []
    for i in (0, 2):
        gate = own_ref[i] + theirs_ref[2 - i]
        up = own_ref[i + 1] + theirs_ref[3 - i]
        hidden.append((gate * jax.nn.sigmoid(gate) * up).astype(jnp.bfloat16))
    hidden = jnp.concatenate(hidden, axis=1)
    parts = BLOCK // LANES
    for b in range(rows // parts):
        at = pl.ds(b * BLOCK, BLOCK)
        out = jnp.dot(hidden, down_ref[:, at], preferred_element_type=jnp.float32)
        for i in range(parts):
            row = pl.ds(b * parts + i, slots, stride=rows)
            rows_ref[row, :] = out[:, i * LANES : (i + 1) * LANES]
    out_ref[...] = rows_ref[...].reshape(out_ref.shape).astype(jnp.bfloat16)


GRANT = pltpu.CompilerParams(vmem_limit_bytes=16 * 2**20)
VMEM = pl.BlockSpec(memory_space=pltpu.VMEM)
HBM = pl.BlockSpec(memory_space=pltpu.HBM)


def in_vmem(x):
    return pltpu.with_memory_space_constraint(x, pltpu.VMEM)


def in_hbm(x):
    return pltpu.with_memory_space_constraint(x, pltpu.HBM)


def body(tokens, norm_gain, token_expert_index, group_prob, expert_weight, w_gate, w_up, w_down):
    rows_here, width = tokens.shape
    topk = token_expert_index.shape[1]
    experts = lax.axis_size("ep")
    tp_count = lax.axis_size("tp")
    chips = tp_count // 2
    share = width // tp_count
    half = width // 2
    units = w_gate.shape[2]
    swap = [(i, i ^ 1) for i in range(tp_count)]
    same_core = [[2 * i + c for i in range(chips)] for c in range(2)]
    per_group = experts // GROUPS
    capacity = min(rows_here, max(2, rows_here * topk // max(per_group - topk, 1) + 1))
    slots_total = experts * capacity
    gates = group_prob[:, None] * expert_weight / jnp.sum(expert_weight, axis=-1, keepdims=True)
    flattened_index = token_expert_index.reshape(-1)
    onehot = (flattened_index[:, None] == jnp.arange(experts, dtype=jnp.int32)[None, :]).astype(
        jnp.int32
    )
    earlier = jnp.cumsum(onehot, axis=0) - onehot
    slot_rank = jnp.sum(earlier * onehot, axis=1)
    place = flattened_index * capacity + slot_rank
    at_place = jnp.arange(slots_total, dtype=jnp.int32)[:, None] == place[None, :]

    weigh = jnp.sum(
        (at_place.astype(jnp.float32) * gates.reshape(-1)[None, :]).reshape(
            slots_total, rows_here, topk
        ),
        axis=2,
    )

    weights = [in_hbm(w[0]) for w in (w_gate, w_up, w_down)]
    lanes = [pltpu.VMEM((slots_total * chips, LANES), jnp.float32)] * (share // LANES)
    outgoing = pl.pallas_call(
        dispatch_kernel,
        out_shape=jax.ShapeDtypeStruct((experts, capacity, chips, share), jnp.bfloat16),
        in_specs=[HBM, HBM, HBM],
        out_specs=VMEM,
        scratch_shapes=[
            pltpu.SMEM((topk, rows_here), jnp.int32),
            pltpu.VMEM((rows_here, width), jnp.bfloat16),
            pltpu.VMEM((1, width), jnp.float32),
            pltpu.SMEM((experts,), jnp.int32),
            pltpu.SemaphoreType.DMA((3,)),
            *[pltpu.VMEM((rows_here * chips, LANES), jnp.float32)] * (share // LANES),
        ],
        compiler_params=GRANT,
        name="dispatch",
    )(*(in_hbm(x) for x in (token_expert_index.T, tokens, norm_gain[None, :])))
    outgoing = outgoing.reshape(experts, capacity * chips, share)
    near, far, cross = pl.pallas_call(
        fetch_kernel,
        out_shape=(
            pltpu.VMEM((2, chips, share, units), jnp.bfloat16),
            jax.ShapeDtypeStruct((2, chips, share, units), jnp.bfloat16),
            jax.ShapeDtypeStruct((units, half), jnp.bfloat16),
        ),
        in_specs=[HBM, HBM, HBM],
        out_specs=(VMEM, VMEM, VMEM),
        scratch_shapes=[
            pltpu.SemaphoreType.DMA((2, chips)),
            pltpu.SemaphoreType.DMA((2, chips)),
            pltpu.SemaphoreType.DMA((chips,)),
        ],
        compiler_params=GRANT,
        name="fetch",
    )(*weights)
    far = lax.ppermute(far, "tp", swap)
    cross = lax.ppermute(cross, "tp", swap)
    arrived = lax.all_to_all(outgoing, "ep", split_axis=0, concat_axis=0, tiled=True)
    arrived, near, far, cross, weigh = lax.optimization_barrier((arrived, near, far, cross, weigh))
    sums = pl.pallas_call(
        sums_kernel,
        out_shape=pltpu.VMEM((4, slots_total, units), jnp.float32),
        in_specs=[VMEM, VMEM, VMEM],
        out_specs=VMEM,
        scratch_shapes=lanes,
        compiler_params=GRANT,
        name="sums",
    )(*(in_vmem(x) for x in (arrived.reshape(slots_total, chips, share), near, far)))
    theirs = lax.ppermute(sums, "tp", swap)
    down = pl.pallas_call(
        down_kernel,
        out_shape=pltpu.VMEM((2 * units, half), jnp.bfloat16),
        in_specs=[HBM, HBM],
        out_specs=VMEM,
        scratch_shapes=[pltpu.SemaphoreType.DMA((chips,)), pltpu.SemaphoreType.DMA],
        compiler_params=GRANT,
        name="down",
    )(weights[2], in_hbm(cross))
    rows = half // LANES
    mine = pl.pallas_call(
        output_kernel,
        out_shape=pltpu.VMEM((slots_total, rows, LANES), jnp.bfloat16),
        in_specs=[VMEM, VMEM, VMEM],
        out_specs=VMEM,
        scratch_shapes=[pltpu.VMEM((slots_total * rows, LANES), jnp.float32)],
        compiler_params=GRANT,
        name="output",
    )(*(in_vmem(x) for x in (sums, theirs, down)))
    mine = mine.reshape(experts, capacity * rows, LANES)
    returned = lax.all_to_all(mine, "ep", split_axis=0, concat_axis=0, tiled=True)
    returned = returned.reshape(slots_total, half)
    partial_mix = jnp.dot(
        weigh.T,
        returned.astype(jnp.float32),
        precision=lax.Precision.HIGHEST,
        preferred_element_type=jnp.float32,
    ).astype(jnp.bfloat16)
    blocks = jnp.moveaxis(partial_mix.reshape(rows_here, chips, share), 1, 0)
    parts = lax.all_to_all(
        blocks, "tp", split_axis=0, concat_axis=0, tiled=True, axis_index_groups=same_core
    )
    return parts.astype(jnp.float32).sum(axis=0).astype(jnp.bfloat16)


def solution(mesh):
    return jax.shard_map(
        body,
        mesh=mesh,
        in_specs=(
            P("ep", None),
            P(),
            P("ep", None),
            P("ep"),
            P("ep", None),
            P("ep", None, "tp"),
            P("ep", None, "tp"),
            P("ep", "tp", None),
        ),
        out_specs=P("ep", "tp"),
        check_vma=False,
    )
```

```python
import jax
import jax.numpy as jnp
from jax import lax
from jax.experimental import pallas as pl
from jax.experimental.pallas import tpu as pltpu
from jax.sharding import PartitionSpec as P

GROUPS = 2
BLOCK = 256
LANES = 128


def block_at(b, which):
    return pl.ds(pl.multiple_of((2 * b + which) * BLOCK, BLOCK), BLOCK)


def into_blocks(gate_hbm, up_hbm, which, out_ref, sems):
    return [
        pltpu.make_async_copy(hbm.at[block_at(b, which)], out_ref.at[i, b], sems.at[i, b])
        for b in range(out_ref.shape[1])
        for i, hbm in enumerate((gate_hbm, up_hbm))
    ]


def columns(hbm, which, out_ref, sems):
    return [
        pltpu.make_async_copy(
            hbm.at[:, block_at(b, which)], out_ref.at[:, b * BLOCK : (b + 1) * BLOCK], sems.at[b]
        )
        for b in range(out_ref.shape[1] // BLOCK)
    ]


def dispatch_kernel(
    index_hbm, tokens_hbm, gain_hbm,
    out_ref,
    index_ref, tokens_ref, gain_ref, count_ref, sems, *lanes,
):
    core = lax.axis_index("tp") % 2
    tokens, width = tokens_ref.shape
    experts, _, chips, share = out_ref.shape
    topk = index_ref.shape[0]
    copies = [
        pltpu.make_async_copy(hbm, ref, sems.at[i])
        for i, (hbm, ref) in enumerate(
            ((tokens_hbm, tokens_ref), (index_hbm, index_ref), (gain_hbm, gain_ref))
        )
    ]
    for copy in copies:
        copy.start()
    out_ref[...] = jnp.zeros_like(out_ref)

    def clear(e, _):
        count_ref[e] = 0

    lax.fori_loop(0, experts, clear, None, unroll=8)
    for copy in copies:
        copy.wait()
    xf = tokens_ref[...].astype(jnp.float32)
    scale = lax.rsqrt(jnp.mean(xf * xf, axis=-1, keepdims=True) + 1e-06)
    for b in range(chips):
        at = block_at(b, core)
        block = tokens_ref[:, at].astype(jnp.float32) * scale * gain_ref[:, at]
        for i, ref in enumerate(lanes):
            ref[pl.ds(b, tokens, stride=chips), :] = block[:, i * LANES : (i + 1) * LANES]

    def token(t, _):
        here = pl.ds(pl.multiple_of(t * chips, chips), chips)
        row = jnp.concatenate([ref[here, :] for ref in lanes], axis=1).astype(jnp.bfloat16)
        for k in range(topk):
            e = index_ref[k, t]
            rank = count_ref[e]
            count_ref[e] = rank + 1
            out_ref[e, rank] = row

    lax.fori_loop(0, tokens, token, None, unroll=True)


def fetch_kernel(
    gate_hbm, up_hbm, down_hbm, near_ref, far_ref, cross_ref, near_sems, far_sems, cross_sems
):
    core = lax.axis_index("tp") % 2
    copies = into_blocks(gate_hbm, up_hbm, 1 - core, far_ref, far_sems)
    copies += columns(down_hbm, 1 - core, cross_ref, cross_sems)
    copies += into_blocks(gate_hbm, up_hbm, core, near_ref, near_sems)
    for copy in copies:
        copy.start()
    for copy in copies:
        copy.wait()


def sums_kernel(x_ref, near_ref, far_ref, sums_ref, *lanes):
    slots, chips, share = x_ref.shape
    for i, ref in enumerate(lanes):
        part = x_ref[:, :, i * LANES : (i + 1) * LANES].astype(jnp.float32)
        ref[...] = part.reshape(slots * chips, LANES)
    sums = [jnp.zeros(sums_ref.shape[1:], jnp.float32)] * 4
    for b in range(chips):
        rows = pl.ds(b, slots, stride=chips)
        x = jnp.concatenate([ref[rows, :] for ref in lanes], axis=1).astype(jnp.bfloat16)
        for i in range(4):
            w = (near_ref, far_ref)[i // 2][i % 2, b]
            sums[i] += jnp.dot(x, w, preferred_element_type=jnp.float32)
    for i in range(4):
        sums_ref[i] = sums[i]


def down_kernel(down_hbm, crossed_hbm, out_ref, sems, sem):
    units = down_hbm.shape[0]
    copies = columns(down_hbm, lax.axis_index("tp") % 2, out_ref.at[:units], sems)
    copies.append(pltpu.make_async_copy(crossed_hbm, out_ref.at[units:], sem))
    for copy in copies:
        copy.start()
    for copy in copies:
        copy.wait()


def output_kernel(own_ref, theirs_ref, down_ref, out_ref, *lanes):
    slots, chips, share = out_ref.shape
    hidden = []
    for i in (0, 2):
        gate = own_ref[i] + theirs_ref[2 - i]
        up = own_ref[i + 1] + theirs_ref[3 - i]
        hidden.append((gate * jax.nn.sigmoid(gate) * up).astype(jnp.bfloat16))
    hidden = jnp.concatenate(hidden, axis=1)
    for b in range(chips):
        at = pl.ds(b * BLOCK, BLOCK)
        out = jnp.dot(hidden, down_ref[:, at], preferred_element_type=jnp.float32)
        for i, ref in enumerate(lanes):
            ref[pl.ds(b, slots, stride=chips), :] = out[:, i * LANES : (i + 1) * LANES]
    for i, ref in enumerate(lanes):
        part = ref[...].reshape(slots, chips, LANES).astype(jnp.bfloat16)
        out_ref[:, :, i * LANES : (i + 1) * LANES] = part


GRANT = pltpu.CompilerParams(vmem_limit_bytes=16 * 2**20)
VMEM = pl.BlockSpec(memory_space=pltpu.VMEM)
HBM = pl.BlockSpec(memory_space=pltpu.HBM)


def in_vmem(x):
    return pltpu.with_memory_space_constraint(x, pltpu.VMEM)


def in_hbm(x):
    return pltpu.with_memory_space_constraint(x, pltpu.HBM)


def body(tokens, norm_gain, token_expert_index, group_prob, expert_weight, w_gate, w_up, w_down):
    rows_here, width = tokens.shape
    topk = token_expert_index.shape[1]
    experts = lax.axis_size("ep")
    tp_count = lax.axis_size("tp")
    chips = tp_count // 2
    share = width // tp_count
    half = width // 2
    units = w_gate.shape[2]
    swap = [(i, i ^ 1) for i in range(tp_count)]
    same_core = [[2 * i + c for i in range(chips)] for c in range(2)]
    per_group = experts // GROUPS
    capacity = min(rows_here, max(2, rows_here * topk // max(per_group - topk, 1) + 1))
    slots_total = experts * capacity
    gates = group_prob[:, None] * expert_weight / jnp.sum(expert_weight, axis=-1, keepdims=True)
    flattened_index = token_expert_index.reshape(-1)
    onehot = (flattened_index[:, None] == jnp.arange(experts, dtype=jnp.int32)[None, :]).astype(
        jnp.int32
    )
    earlier = jnp.cumsum(onehot, axis=0) - onehot
    slot_rank = jnp.sum(earlier * onehot, axis=1)
    place = flattened_index * capacity + slot_rank
    at_place = jnp.arange(slots_total, dtype=jnp.int32)[:, None] == place[None, :]

    weigh = jnp.sum(
        (at_place.astype(jnp.float32) * gates.reshape(-1)[None, :]).reshape(
            slots_total, rows_here, topk
        ),
        axis=2,
    )

    weights = [in_hbm(w[0]) for w in (w_gate, w_up, w_down)]
    lanes = [pltpu.VMEM((slots_total * chips, LANES), jnp.float32)] * (share // LANES)
    outgoing = pl.pallas_call(
        dispatch_kernel,
        out_shape=jax.ShapeDtypeStruct((experts, capacity, chips, share), jnp.bfloat16),
        in_specs=[HBM, HBM, HBM],
        out_specs=VMEM,
        scratch_shapes=[
            pltpu.SMEM((topk, rows_here), jnp.int32),
            pltpu.VMEM((rows_here, width), jnp.bfloat16),
            pltpu.VMEM((1, width), jnp.float32),
            pltpu.SMEM((experts,), jnp.int32),
            pltpu.SemaphoreType.DMA((3,)),
            *[pltpu.VMEM((rows_here * chips, LANES), jnp.float32)] * (share // LANES),
        ],
        compiler_params=GRANT,
        name="dispatch",
    )(*(in_hbm(x) for x in (token_expert_index.T, tokens, norm_gain[None, :])))
    outgoing = outgoing.reshape(experts, capacity * chips, share)
    near, far, cross = pl.pallas_call(
        fetch_kernel,
        out_shape=(
            pltpu.VMEM((2, chips, share, units), jnp.bfloat16),
            jax.ShapeDtypeStruct((2, chips, share, units), jnp.bfloat16),
            jax.ShapeDtypeStruct((units, half), jnp.bfloat16),
        ),
        in_specs=[HBM, HBM, HBM],
        out_specs=(VMEM, VMEM, VMEM),
        scratch_shapes=[
            pltpu.SemaphoreType.DMA((2, chips)),
            pltpu.SemaphoreType.DMA((2, chips)),
            pltpu.SemaphoreType.DMA((chips,)),
        ],
        compiler_params=GRANT,
        name="fetch",
    )(*weights)
    far = lax.ppermute(far, "tp", swap)
    cross = lax.ppermute(cross, "tp", swap)
    arrived = lax.all_to_all(outgoing, "ep", split_axis=0, concat_axis=0, tiled=True)
    arrived, near, far, cross, weigh = lax.optimization_barrier((arrived, near, far, cross, weigh))
    sums = pl.pallas_call(
        sums_kernel,
        out_shape=pltpu.VMEM((4, slots_total, units), jnp.float32),
        in_specs=[VMEM, VMEM, VMEM],
        out_specs=VMEM,
        scratch_shapes=lanes,
        compiler_params=GRANT,
        name="sums",
    )(*(in_vmem(x) for x in (arrived.reshape(slots_total, chips, share), near, far)))
    theirs = lax.ppermute(sums, "tp", swap)
    down = pl.pallas_call(
        down_kernel,
        out_shape=pltpu.VMEM((2 * units, half), jnp.bfloat16),
        in_specs=[HBM, HBM],
        out_specs=VMEM,
        scratch_shapes=[pltpu.SemaphoreType.DMA((chips,)), pltpu.SemaphoreType.DMA],
        compiler_params=GRANT,
        name="down",
    )(weights[2], in_hbm(cross))
    mine = pl.pallas_call(
        output_kernel,
        out_shape=pltpu.VMEM((slots_total, chips, share), jnp.bfloat16),
        in_specs=[VMEM, VMEM, VMEM],
        out_specs=VMEM,
        scratch_shapes=lanes,
        compiler_params=GRANT,
        name="output",
    )(*(in_vmem(x) for x in (sums, theirs, down)))
    mine = mine.reshape(experts, capacity * chips, share)
    returned = lax.all_to_all(mine, "ep", split_axis=0, concat_axis=0, tiled=True)
    returned = returned.reshape(slots_total, half)
    partial_mix = jnp.dot(
        weigh.T,
        returned.astype(jnp.float32),
        precision=lax.Precision.HIGHEST,
        preferred_element_type=jnp.float32,
    ).astype(jnp.bfloat16)
    blocks = jnp.moveaxis(partial_mix.reshape(rows_here, chips, share), 1, 0)
    parts = lax.all_to_all(
        blocks, "tp", split_axis=0, concat_axis=0, tiled=True, axis_index_groups=same_core
    )
    return parts.astype(jnp.float32).sum(axis=0).astype(jnp.bfloat16)


def solution(mesh):
    return jax.shard_map(
        body,
        mesh=mesh,
        in_specs=(
            P("ep", None),
            P(),
            P("ep", None),
            P("ep"),
            P("ep", None),
            P("ep", None, "tp"),
            P("ep", None, "tp"),
            P("ep", "tp", None),
        ),
        out_specs=P("ep", "tp"),
        check_vma=False,
    )
```
